128 devices in a mesh: st: 64 (over z, y, x), tp: 2 (over core).
Axes of the slice: x: 4, y: 4, z: 4, core: 2. Of those that a mesh axis runs over, the one named last changes fastest.
Arguments:
- hidden: bfloat16 [32768, 2048], P('st'), may hold values from -24 to 24
- passage_store: bfloat16 [2048, 64, 2048], P('st'), may hold values from -6 to 6
- passage_ids: int32 [512, 4], P('st'), may hold values from 0 to 2047, as said below
- query_weight: bfloat16 [2048, 512], P(None, 'tp'), may hold values from -0.125 to 0.125
- gate_weight: bfloat16 [2048, 512], P(None, 'tp'), may hold values from -0.125 to 0.125
- key_weight: bfloat16 [2048, 512], P(None, 'tp'), may hold values from -0.125 to 0.125
- value_weight: bfloat16 [2048, 512], P(None, 'tp'), may hold values from -0.125 to 0.125
- output_grad: bfloat16 [32768, 512], P('st', 'tp'), may hold values from -6 to 6
Outputs:
- grad_hidden: bfloat16 [32768, 2048], P(('st', 'tp'))
- grad_store: bfloat16 [2048, 64, 2048], P(('st', 'tp'))
- grad_value_weight: float32 [2048, 512], P(None, 'tp')
The draws below stay inside these ranges and needn't reach their ends.
Inputs may be any that keep to these rules, and one draw needn't show every extreme that they name: `passage_ids`: passage p is held at st index p // 32. The 32 ids of one index of st (its 8 blocks) are distinct; at most 1 of them name passages of one owner, and on every index some owner is named exactly 1 times. Every index reads at least one passage of the owner before it, of the owner after it and of the owner half the axis away.
All inputs are finite; a program needn't handle non-finite values.
Results may differ from the reference program's by a relative error of at most 0.012.
The reference program's roundings to bfloat16 on the way count: a program that leaves them out, or rounds other values in their place, can miss the bound.
Values may be sent and summed in bfloat16 or wider, within the bound.
No kernel may reach another device: no remote copies, remote signals or barrier semaphores. Data moves between devices by JAX's collectives and lax.ppermute only.
A program may use at most 128 MiB of HBM per device.

```python
import jax
import jax.numpy as jnp
from jax import lax

D = 2048
HEADS = 2
HEAD_DIM = 256
MW = 512
BLK = 64
NP = 4
PLEN = 64
P_DEV = 32
TOKENS = 32768
PASSAGES = 2048
NB_DEV = 8
NBLK = 512
REQ_DEV = 32
CAP = 1


def draw_hidden(key, part):
    keys_three = jax.random.split(key, 3)
    drawn = jnp.clip(jax.random.normal(keys_three[0], (TOKENS, D), jnp.float32), -6.0, 6.0)
    return drawn.astype(jnp.bfloat16)


def draw_passage_ids(key, part):
    owner_total = PASSAGES // P_DEV
    slot_total = owner_total * CAP

    def one_source(source_key, source):
        split_keys = jax.random.split(source_key, 4)
        slot_iota = jnp.arange(slot_total, dtype=jnp.int32)
        slot_owner = slot_iota // CAP
        slot_rank = slot_iota % CAP
        shuffled = jax.random.permutation(split_keys[0], slot_total).astype(jnp.int32)
        before = (source + owner_total - 1) % owner_total
        after = (source + 1) % owner_total
        across = (source + owner_total // 2) % owner_total
        score = jnp.where(slot_owner == before, slot_rank, shuffled + 2 * slot_total)
        score = jnp.where((slot_owner == across) & (slot_rank == 0), CAP, score)
        score = jnp.where((slot_owner == after) & (slot_rank == 0), CAP + 1, score)
        chosen = jnp.argsort(score, stable=True)[:REQ_DEV].astype(jnp.int32)
        chosen_owner = chosen // CAP
        chosen_rank = chosen % CAP
        first_pick = jax.random.randint(split_keys[1], (owner_total,), 0, P_DEV)
        second_pick = jax.random.randint(split_keys[2], (owner_total,), 0, P_DEV)
        popular = jnp.minimum(first_pick, second_pick)
        local_index = (popular[chosen_owner] + chosen_rank) % P_DEV
        ids_flat = jax.random.permutation(split_keys[3], chosen_owner * P_DEV + local_index)
        return ids_flat.reshape(NB_DEV, NP).astype(jnp.int32)
    source_keys = jax.random.split(key, owner_total)
    return jax.vmap(one_source)(source_keys, jnp.arange(owner_total, dtype=jnp.int32)).reshape(NBLK, NP)


def level_of(stream_key, extent, cuts, smallest, largest):
    def one(axis_at, parts):
        heights = jax.random.uniform(jax.random.fold_in(jax.random.fold_in(stream_key, 6), axis_at), (parts,), jnp.float32, smallest / len(cuts), largest / len(cuts))
        return jnp.repeat(jnp.exp(heights), extent[axis_at] // parts).reshape((-1,) + (1,) * (len(extent) - axis_at - 1))

    factor_of = one(*cuts[0])
    for cut in cuts[1:]:
        factor_of = factor_of * one(*cut)
    return factor_of


def noise(rng, extent, width, reach, cuts=(), kind=jnp.bfloat16):
    array = width * jax.random.normal(rng, extent, jnp.float32)
    if cuts:
        array = array * level_of(rng, extent, cuts, -0.22, 0.18)
    return jnp.clip(array, -reach, reach).astype(kind)


def setup_inputs(seed: int = 0) -> dict:
    key_list = jax.random.split(jax.random.key(seed), 9)
    return {
        "hidden": draw_hidden(jax.random.fold_in(key_list[8], 71), 0),
        "passage_store": noise(key_list[1], (PASSAGES, PLEN, D), 1.0, 6.0, ((0, 64),)),
        "passage_ids": draw_passage_ids(jax.random.fold_in(key_list[8], 71), 0),
        "query_weight": noise(key_list[3], (D, MW), D ** -0.5, 0.125, ((1, 2),)),
        "gate_weight": noise(key_list[4], (D, MW), D ** -0.5, 0.125, ((1, 2),)),
        "key_weight": noise(key_list[5], (D, MW), D ** -0.5, 0.125, ((1, 2),)),
        "value_weight": noise(key_list[6], (D, MW), D ** -0.5, 0.125, ((1, 2),)),
        "output_grad": noise(key_list[7], (TOKENS, MW), 1.0, 6.0, ((0, 64), (1, 2))),
    }


def block_grads(operands):
    query_block, gate_block, upstream_block, key_block, value_block = operands
    score_scale = HEAD_DIM ** -0.5
    query_heads = query_block.astype(jnp.float32).reshape(BLK, HEADS, HEAD_DIM)
    key_heads = key_block.astype(jnp.float32).reshape(NP * PLEN, HEADS, HEAD_DIM)
    value_heads = value_block.astype(jnp.float32).reshape(NP * PLEN, HEADS, HEAD_DIM)
    scores = jnp.einsum('qhd,khd->hqk', query_heads, key_heads) * score_scale
    probs = jax.nn.softmax(scores, axis=-1)
    probs_low = probs.astype(jnp.bfloat16)
    attended = jnp.einsum('hqk,khd->qhd', probs_low.astype(jnp.float32), value_heads).reshape(BLK, MW)
    gate_sigmoid = jax.nn.sigmoid(gate_block)
    upstream = upstream_block.astype(jnp.float32)
    d_attended = (upstream * gate_block * gate_sigmoid).astype(jnp.bfloat16)
    d_gates = (upstream * attended * gate_sigmoid * (1.0 + gate_block * (1.0 - gate_sigmoid))).astype(jnp.bfloat16)
    d_heads = d_attended.astype(jnp.float32).reshape(BLK, HEADS, HEAD_DIM)
    d_probs = jnp.einsum('qhd,khd->hqk', d_heads, value_heads)
    centre = jnp.sum(probs * d_probs, axis=-1, keepdims=True)
    d_scores = (probs * (d_probs - centre) * score_scale).astype(jnp.bfloat16).astype(jnp.float32)
    d_queries = jnp.einsum('hqk,khd->qhd', d_scores, key_heads).reshape(BLK, MW).astype(jnp.bfloat16)
    d_block_keys = jnp.einsum('hqk,qhd->khd', d_scores, query_heads).reshape(NP, PLEN, MW)
    d_block_values = jnp.einsum('hqk,qhd->khd', probs_low.astype(jnp.float32), d_heads).reshape(NP, PLEN, MW)
    return d_queries, d_gates, d_block_keys, d_block_values


def reference(hidden, passage_store, passage_ids, query_weight, gate_weight, key_weight, value_weight, output_grad):
    store_rows = passage_store.reshape(PASSAGES * PLEN, D)
    keys = jnp.dot(store_rows, key_weight, preferred_element_type=jnp.float32).astype(jnp.bfloat16).reshape(PASSAGES, PLEN, MW)
    values = jnp.dot(store_rows, value_weight, preferred_element_type=jnp.float32).astype(jnp.bfloat16).reshape(PASSAGES, PLEN, MW)
    queries = jnp.dot(hidden, query_weight, preferred_element_type=jnp.float32).astype(jnp.bfloat16).reshape(NBLK, BLK, MW)
    gates = jnp.dot(hidden, gate_weight, preferred_element_type=jnp.float32).reshape(NBLK, BLK, MW)
    flat_ids = passage_ids.reshape(NBLK * NP).astype(jnp.int32)
    key_blocks = keys[flat_ids].reshape(NBLK, NP * PLEN, MW)
    value_blocks = values[flat_ids].reshape(NBLK, NP * PLEN, MW)
    d_queries, d_gates, d_block_keys, d_block_values = lax.map(
        block_grads, (queries, gates, output_grad.reshape(NBLK, BLK, MW), key_blocks, value_blocks))
    d_queries = d_queries.reshape(TOKENS, MW)
    d_gates = d_gates.reshape(TOKENS, MW)
    grad_hidden = (jnp.dot(d_queries, query_weight.T, preferred_element_type=jnp.float32)
                   + jnp.dot(d_gates, gate_weight.T, preferred_element_type=jnp.float32)).astype(jnp.bfloat16)
    key_totals = jnp.zeros((PASSAGES, PLEN, MW), jnp.float32).at[flat_ids].add(d_block_keys.reshape(NBLK * NP, PLEN, MW))
    value_totals = jnp.zeros((PASSAGES, PLEN, MW), jnp.float32).at[flat_ids].add(d_block_values.reshape(NBLK * NP, PLEN, MW))
    key_low = key_totals.astype(jnp.bfloat16).reshape(PASSAGES * PLEN, MW)
    value_low = value_totals.astype(jnp.bfloat16).reshape(PASSAGES * PLEN, MW)
    grad_store = (jnp.dot(key_low, key_weight.T, preferred_element_type=jnp.float32)
                  + jnp.dot(value_low, value_weight.T, preferred_element_type=jnp.float32)).astype(jnp.bfloat16).reshape(PASSAGES, PLEN, D)
    grad_value_weight = jnp.dot(store_rows.T, value_low, preferred_element_type=jnp.float32)
    return grad_hidden, grad_store, grad_value_weight
```

```python
import functools

import jax
import jax.numpy as jnp
from jax import lax
from jax.experimental import pallas as pl
from jax.experimental.pallas import tpu as pltpu
from jax.sharding import PartitionSpec as P

HEAD_DIM = 256
F32 = jnp.float32
BF16 = jnp.bfloat16
VMEM = pl.BlockSpec(memory_space=pltpu.VMEM)
SMEM = pl.BlockSpec(memory_space=pltpu.SMEM)


def dot(a, b, ca, cb):
    return lax.dot_general(a, b, (((ca,), (cb,)), ((), ())), preferred_element_type=F32)


def swap_tp(x):
    return lax.ppermute(x, "tp", [(0, 1), (1, 0)])


def exchange(x):
    return lax.all_to_all(x, "st", split_axis=0, concat_axis=0, tiled=True)


def pick_kernel(wanted_ref, rows_ref, out_ref):
    def step(i, carry):
        out_ref[i] = rows_ref[jnp.maximum(wanted_ref[i, 0] - 1, 0)]
        return carry

    lax.fori_loop(0, out_ref.shape[0], step, 0, unroll=8)


def pick(wanted, rows):
    return pl.pallas_call(
        pick_kernel,
        out_shape=jax.ShapeDtypeStruct((wanted.shape[0], *rows.shape[1:]), rows.dtype),
        in_specs=[SMEM, VMEM],
        out_specs=VMEM,
        name="pick",
    )(wanted, rows)


def probs_kernel(held, ids_ref, q_ref, da_ref, k_ref, p_ref, dv_ref):
    blocks, per = ids_ref.shape
    rows = q_ref.shape[0] // blocks
    span = k_ref.shape[1]
    scale = HEAD_DIM**-0.5
    for b in range(blocks):
        mine = slice(b * rows, (b + 1) * rows)
        owner = [lax.div(ids_ref[b, j], held) for j in range(per)]
        k = jnp.concatenate([k_ref[o] for o in owner], axis=0)
        s = dot(q_ref[mine], k, 1, 1) * scale
        e = jnp.exp(s - jnp.max(s, axis=1, keepdims=True))
        p = e / jnp.sum(e, axis=1, keepdims=True)
        p_ref[mine] = p
        dv = dot(p.astype(BF16), da_ref[mine], 0, 0).astype(BF16)
        for j in range(per):
            dv_ref[owner[j]] = dv[j * span : (j + 1) * span]


def grads_kernel(held, ids_ref, tp_ref, q_ref, da_ref, g_ref, og_ref, p_ref, k_ref, v_ref, keep_ref, send_ref, dk_ref):
    blocks, per = ids_ref.shape
    rows = q_ref.shape[0] // blocks
    span = k_ref.shape[1]
    scale = HEAD_DIM**-0.5
    half = blocks // 2
    for n in range(blocks):
        b = lax.rem(n + half * tp_ref[0], blocks)
        mine = pl.ds(pl.multiple_of(b * rows, rows), rows)
        owner = [lax.div(ids_ref[b, j], held) for j in range(per)]
        k = jnp.concatenate([k_ref[o] for o in owner], axis=0)
        v = jnp.concatenate([v_ref[o] for o in owner], axis=0)
        p = p_ref[mine]
        q = q_ref[mine]
        g = g_ref[mine]
        dp = dot(da_ref[mine], v, 1, 1)
        attended = dot(p.astype(BF16), v, 1, 0)
        centre = jnp.sum(p * dp, axis=1, keepdims=True)
        ds = (p * (dp - centre) * scale).astype(BF16)
        dq = dot(ds, k, 1, 0).astype(BF16)
        dk = dot(ds, q, 0, 0).astype(BF16)
        sg = jax.nn.sigmoid(g)
        dg = (og_ref[mine].astype(F32) * attended * sg * (1.0 + g * (1.0 - sg))).astype(BF16)
        for j in range(per):
            dk_ref[owner[j], 0:span] = dk[j * span : (j + 1) * span]
        out = keep_ref if n < half else send_ref
        at = slice((n % half) * rows, (n % half + 1) * rows)
        out[0, at] = dq
        out[1, at] = dg


def add_slots(wanted_ref, tp_ref, came_ref, acc, keep_ref, send_ref):
    span = acc.shape[1]
    acc[...] = jnp.zeros_like(acc)

    def step(i, carry):
        at = wanted_ref[i, 0]
        acc[at] = acc[at] + came_ref[i, 0:span].astype(F32)
        return carry

    lax.fori_loop(0, came_ref.shape[0], step, 0, unroll=8)
    half = keep_ref.shape[0]
    tp = tp_ref[0]
    keep_ref[...] = acc[pl.ds(1 + half * tp, half)].astype(BF16)
    send_ref[...] = acc[pl.ds(1 + half * (1 - tp), half)].astype(BF16)


def value_totals_kernel(wanted_ref, tp_ref, came_ref, keep_ref, send_ref, all_ref, acc):
    add_slots(wanted_ref, tp_ref, came_ref, acc, keep_ref, send_ref)
    held, span, width = acc.shape[0] - 1, acc.shape[1], acc.shape[2]
    for i in range(held):
        all_ref[:, i * span : (i + 1) * span] = acc[1 + i].T.astype(BF16)


def key_totals_kernel(wanted_ref, tp_ref, came_ref, keep_ref, send_ref, part_ref, acc):
    add_slots(wanted_ref, tp_ref, came_ref, acc, keep_ref, send_ref)
    span = acc.shape[1]

    def step(i, carry):
        return carry + came_ref[i, span:].astype(F32)

    count, rows, width = part_ref.shape
    total = lax.fori_loop(0, count, step, jnp.zeros((rows, width), F32), unroll=8).astype(BF16)
    for i in range(count):
        part_ref[i] = total


def weight_kernel(store_ref, vt_ref, buf_ref, out_ref):
    part = dot(vt_ref[...], store_ref[...], 1, 0)
    part = part.T.astype(BF16)
    rows = out_ref.shape[1]
    for i in range(out_ref.shape[0]):
        out_ref[i] = part[i * rows : (i + 1) * rows]


def back_kernel(a0, a1, a2, a3, w0, w1, w2, w3, out_ref):
    a = jnp.concatenate([a0[...], a1[...], a2[...], a3[...]], axis=1)
    step = 256
    for n in range(0, out_ref.shape[1], step):
        w = jnp.concatenate([r[n : n + step] for r in (w0, w1, w2, w3)], axis=1)
        out_ref[:, n : n + step] = dot(a, w, 1, 1).astype(BF16)


def back(parts, weights, tile=256):
    rows, width = parts[0].shape
    depth = weights[0].shape[0]
    return pl.pallas_call(
        back_kernel,
        grid=(rows // tile,),
        out_shape=jax.ShapeDtypeStruct((rows, depth), BF16),
        in_specs=[pl.BlockSpec((tile, width), lambda i: (i, 0))] * 4
        + [pl.BlockSpec((depth, width), lambda i: (0, 0))] * 4,
        out_specs=pl.BlockSpec((tile, depth), lambda i: (i, 0)),
        name="back",
    )(*parts, *weights)


def body(hidden, passage_store, passage_ids, query_weight, gate_weight, key_weight, value_weight, output_grad):
    owners = lax.axis_size("st")
    held, span, depth = passage_store.shape
    blocks, per_block = passage_ids.shape
    width = query_weight.shape[1]
    tokens = hidden.shape[0]
    tp = lax.axis_index("tp").astype(jnp.int32).reshape(1)

    ids = passage_ids.reshape(-1)
    asked = (ids // held)[None, :] == jnp.arange(owners, dtype=jnp.int32)[:, None]
    request = jnp.sum(jnp.where(asked, (ids % held + 1)[None, :], 0), axis=1)
    wanted = exchange(jnp.broadcast_to(request[:, None], (owners, 128)))

    store_rows = passage_store.reshape(held * span, depth)
    keys = jnp.dot(store_rows, key_weight, preferred_element_type=F32).astype(BF16).reshape(held, span, width)
    came_keys = exchange(pick(wanted, keys))
    values = jnp.dot(store_rows, value_weight, preferred_element_type=F32).astype(BF16).reshape(held, span, width)
    came_values = exchange(pick(wanted, values))

    queries = jnp.dot(hidden, query_weight, preferred_element_type=F32).astype(BF16)
    gates = jnp.dot(hidden, gate_weight, preferred_element_type=F32)
    d_attended = (output_grad.astype(F32) * gates * jax.nn.sigmoid(gates)).astype(BF16)

    probs, back_values = pl.pallas_call(
        functools.partial(probs_kernel, held),
        out_shape=(
            jax.ShapeDtypeStruct((tokens, per_block * span), F32),
            jax.ShapeDtypeStruct((owners, span, width), BF16),
        ),
        in_specs=[SMEM, VMEM, VMEM, VMEM],
        out_specs=(VMEM, VMEM),
        name="probs",
    )(passage_ids, queries, d_attended, came_keys)
    came_dvalues = exchange(back_values)

    piece = depth // owners
    half_tokens = jax.ShapeDtypeStruct((2, tokens // 2, width), BF16)
    keep_tokens, send_tokens, back_keys = pl.pallas_call(
        functools.partial(grads_kernel, held),
        out_shape=(half_tokens, half_tokens, jax.ShapeDtypeStruct((owners, span + piece, width), BF16)),
        in_specs=[SMEM, SMEM] + [VMEM] * 7,
        out_specs=(VMEM, VMEM, VMEM),
        name="grads",
    )(passage_ids, tp, queries, d_attended, gates, output_grad, probs, came_keys, came_values)

    half_held = jax.ShapeDtypeStruct((held // 2, span, width), BF16)
    keep_values, send_values, values_across = pl.pallas_call(
        value_totals_kernel,
        out_shape=(half_held, half_held, jax.ShapeDtypeStruct((width, held * span), BF16)),
        in_specs=[SMEM, SMEM, VMEM],
        out_specs=(VMEM, VMEM, VMEM),
        scratch_shapes=[pltpu.VMEM((held + 1, span, width), F32)],
        name="value_totals",
    )(wanted, tp, came_dvalues)

    tile = 256
    back_keys = pl.pallas_call(
        weight_kernel,
        grid=(depth // tile,),
        out_shape=jax.ShapeDtypeStruct(back_keys.shape, BF16),
        in_specs=[
            pl.BlockSpec((held * span, tile), lambda i: (0, i)),
            pl.BlockSpec((width, held * span), lambda i: (0, 0)),
            pl.BlockSpec(memory_space=pl.ANY),
        ],
        out_specs=pl.BlockSpec((tile // piece, piece, width), lambda i: (i, span // piece, 0)),
        input_output_aliases={2: 0},
        name="weight",
    )(store_rows, values_across, back_keys)
    came_dkeys = exchange(back_keys)

    keep_keys, send_keys, summed = pl.pallas_call(
        key_totals_kernel,
        out_shape=(half_held, half_held, jax.ShapeDtypeStruct((owners, piece, width), BF16)),
        in_specs=[SMEM, SMEM, VMEM],
        out_specs=(VMEM, VMEM, VMEM),
        scratch_shapes=[pltpu.VMEM((held + 1, span, width), F32)],
        name="key_totals",
    )(wanted, tp, came_dkeys)
    grad_value_weight = exchange(summed).reshape(depth, width).astype(F32)

    other_query, other_gate, other_key, other_value = (
        swap_tp(w) for w in (query_weight, gate_weight, key_weight, value_weight)
    )
    other_tokens = swap_tp(send_tokens)
    other_values = swap_tp(send_values)
    other_keys = swap_tp(send_keys)
    grad_hidden = back(
        (keep_tokens[0], other_tokens[0], keep_tokens[1], other_tokens[1]),
        (query_weight, other_query, gate_weight, other_gate),
    )
    rows = held // 2 * span
    grad_store = back(
        tuple(t.reshape(rows, width) for t in (keep_keys, other_keys, keep_values, other_values)),
        (key_weight, other_key, value_weight, other_value),
    ).reshape(held // 2, span, depth)
    return grad_hidden, grad_store, grad_value_weight


def solution(mesh):
    placed = (
        P("st", None),
        P("st", None, None),
        P("st", None),
        P(None, "tp"),
        P(None, "tp"),
        P(None, "tp"),
        P(None, "tp"),
        P("st", "tp"),
    )
    return jax.shard_map(
        body,
        mesh=mesh,
        in_specs=placed,
        out_specs=(P(("st", "tp"), None), P(("st", "tp"), None, None), P(None, "tp")),
        check_vma=False,
    )
```

```python
import functools

import jax
import jax.numpy as jnp
from jax import lax
from jax.experimental import pallas as pl
from jax.experimental.pallas import tpu as pltpu
from jax.sharding import PartitionSpec as P

HEAD_DIM = 256
PAUSE = 2850
F32 = jnp.float32
BF16 = jnp.bfloat16
VMEM = pl.BlockSpec(memory_space=pltpu.VMEM)
SMEM = pl.BlockSpec(memory_space=pltpu.SMEM)
ANY = pl.BlockSpec(memory_space=pl.ANY)


def dot(a, b, ca, cb):
    return lax.dot_general(a, b, (((ca,), (cb,)), ((), ())), preferred_element_type=F32)


def swap_tp(x):
    return lax.ppermute(x, "tp", [(0, 1), (1, 0)])


def exchange(x):
    return lax.all_to_all(x, "st", split_axis=0, concat_axis=0, tiled=True)


def request_kernel(held, ids_ref, out_ref):
    per, blocks = ids_ref.shape
    out_ref[...] = jnp.zeros_like(out_ref)
    for b in range(blocks):
        for j in range(per):
            at = ids_ref[j, b]
            owner = lax.div(at, held)
            out_ref[pl.ds(owner, 1)] = jnp.full((1, out_ref.shape[1]), at - owner * held + 1, jnp.int32)


def pick_kernel(wanted_ref, pause_ref, rows_ref, *refs):
    out_ref, wait, sem = refs[-3:]
    if pause_ref is not None:
        wait[...] = lax.fori_loop(0, pause_ref[0], lambda i, c: jnp.tanh(c), jnp.zeros(wait.shape, F32))

    def step(i, carry):
        at = jnp.maximum(wanted_ref[i, 0] - 1, 0)
        pltpu.make_async_copy(rows_ref.at[at], out_ref.at[i], sem).start()
        return carry

    lax.fori_loop(0, out_ref.shape[0], step, 0, unroll=8)
    pltpu.make_async_copy(out_ref, out_ref, sem).wait()


def pick(wanted, pause, rows, *after):
    return pl.pallas_call(
        pick_kernel,
        out_shape=jax.ShapeDtypeStruct((wanted.shape[0], *rows.shape[1:]), rows.dtype),
        in_specs=[SMEM, SMEM, VMEM] + [ANY] * len(after),
        out_specs=ANY,
        scratch_shapes=[pltpu.VMEM((8, 128), F32), pltpu.SemaphoreType.DMA],
        name="pick",
    )(wanted, pause, rows, *after)


def probs_kernel(held, ids_ref, q_ref, da_ref, k_ref, p_ref, dv_ref):
    per, blocks = ids_ref.shape
    rows = q_ref.shape[0] // blocks
    span = k_ref.shape[1]
    scale = HEAD_DIM**-0.5
    for b in range(blocks):
        mine = slice(b * rows, (b + 1) * rows)
        owner = [lax.div(ids_ref[j, b], held) for j in range(per)]
        k = jnp.concatenate([k_ref[o] for o in owner], axis=0)
        s = dot(q_ref[mine], k, 1, 1) * scale
        e = jnp.exp(s - jnp.max(s, axis=1, keepdims=True))
        p = e / jnp.sum(e, axis=1, keepdims=True)
        p_ref[mine] = p
        dv = dot(p.astype(BF16), da_ref[mine], 0, 0).astype(BF16)
        for j in range(per):
            dv_ref[owner[j]] = dv[j * span : (j + 1) * span]


def grads_kernel(held, ids_ref, tp_ref, q_ref, da_ref, g_ref, og_ref, p_ref, k_ref, v_ref, keep_dq, keep_dg, send_dq, send_dg, dk_ref):
    per, blocks = ids_ref.shape
    rows = q_ref.shape[0] // blocks
    span = k_ref.shape[1]
    scale = HEAD_DIM**-0.5
    half = blocks // 2
    for n in range(blocks):
        b = lax.rem(n + half * tp_ref[0], blocks)
        mine = pl.ds(pl.multiple_of(b * rows, rows), rows)
        owner = [lax.div(ids_ref[j, b], held) for j in range(per)]
        k = jnp.concatenate([k_ref[o] for o in owner], axis=0)
        v = jnp.concatenate([v_ref[o] for o in owner], axis=0)
        p = p_ref[mine]
        q = q_ref[mine]
        g = g_ref[mine]
        dp = dot(da_ref[mine], v, 1, 1)
        attended = dot(p.astype(BF16), v, 1, 0)
        centre = jnp.sum(p * dp, axis=1, keepdims=True)
        ds = (p * (dp - centre) * scale).astype(BF16)
        dq = dot(ds, k, 1, 0).astype(BF16)
        dk = dot(ds, q, 0, 0).astype(BF16)
        sg = jax.nn.sigmoid(g)
        dg = (og_ref[mine].astype(F32) * attended * sg * (1.0 + g * (1.0 - sg))).astype(BF16)
        for j in range(per):
            dk_ref[owner[j]] = dk[j * span : (j + 1) * span]
        at = slice((n % half) * rows, (n % half + 1) * rows)
        (keep_dq if n < half else send_dq)[at] = dq
        (keep_dg if n < half else send_dg)[at] = dg


def add_slots(wanted_ref, tp_ref, came_ref, acc, keep_ref, send_ref):
    acc[...] = jnp.zeros_like(acc)

    def step(i, carry):
        at = wanted_ref[i, 0]
        acc[at] = acc[at] + came_ref[i].astype(F32)
        return carry

    lax.fori_loop(0, came_ref.shape[0], step, 0, unroll=8)
    half = keep_ref.shape[0]
    tp = tp_ref[0]
    keep_ref[...] = acc[pl.ds(1 + half * tp, half)].astype(BF16)
    send_ref[...] = acc[pl.ds(1 + half * (1 - tp), half)].astype(BF16)


def add_slots_kernel(wanted_ref, tp_ref, came_ref, keep_ref, send_ref, acc):
    add_slots(wanted_ref, tp_ref, came_ref, acc, keep_ref, send_ref)


def value_totals_kernel(wanted_ref, tp_ref, came_ref, keep_ref, send_ref, all_ref, acc):
    add_slots(wanted_ref, tp_ref, came_ref, acc, keep_ref, send_ref)
    held, span = acc.shape[0] - 1, acc.shape[1]
    for i in range(held):
        all_ref[:, i * span : (i + 1) * span] = acc[1 + i].T.astype(BF16)


def weight_kernel(store_ref, vt_ref, out_ref):
    part = dot(vt_ref[...], store_ref[...], 1, 0).T.astype(BF16)
    rows = out_ref.shape[1]
    for i in range(out_ref.shape[0]):
        out_ref[i] = part[i * rows : (i + 1) * rows]


def back_kernel(terms, *refs):
    out_ref = refs[-1]
    a = jnp.concatenate([r[...] for r in refs[:terms]], axis=1)
    step = 256
    for n in range(0, out_ref.shape[1], step):
        w = jnp.concatenate([r[n : n + step] for r in refs[terms:-1]], axis=1)
        out_ref[:, n : n + step] = dot(a, w, 1, 1).astype(out_ref.dtype)


def back(terms, weights, dtype, tile=256):
    rows, width = terms[0].shape
    depth = weights[0].shape[0]
    return pl.pallas_call(
        functools.partial(back_kernel, len(terms)),
        grid=(rows // tile,),
        out_shape=jax.ShapeDtypeStruct((rows, depth), dtype),
        in_specs=[pl.BlockSpec((tile, width), lambda i: (i, 0))] * len(terms)
        + [pl.BlockSpec((depth, width), lambda i: (0, 0))] * len(weights),
        out_specs=pl.BlockSpec((tile, depth), lambda i: (i, 0)),
        name="back",
    )(*terms, *weights)


def body(hidden, passage_store, passage_ids, query_weight, gate_weight, key_weight, value_weight, output_grad):
    owners = lax.axis_size("st")
    held, span, depth = passage_store.shape
    _, per_block = passage_ids.shape
    width = query_weight.shape[1]
    tokens = hidden.shape[0]
    tp = lax.axis_index("tp").astype(jnp.int32).reshape(1)

    ids = passage_ids.T
    request = pl.pallas_call(
        functools.partial(request_kernel, held),
        out_shape=jax.ShapeDtypeStruct((owners, 128), jnp.int32),
        in_specs=[SMEM],
        out_specs=VMEM,
        name="request",
    )(ids)
    wanted = exchange(request)

    other_key, other_value = swap_tp(key_weight), swap_tp(value_weight)
    store_rows = passage_store.reshape(held * span, depth)
    keys = jnp.dot(store_rows, key_weight, preferred_element_type=F32).astype(BF16).reshape(held, span, width)
    pause = tp * PAUSE
    came_keys = exchange(pick(wanted, pause, keys, other_key, other_value))
    values = jnp.dot(store_rows, value_weight, preferred_element_type=F32).astype(BF16).reshape(held, span, width)
    came_values = exchange(pick(wanted, jnp.zeros_like(tp), values))

    queries = jnp.dot(hidden, query_weight, preferred_element_type=F32).astype(BF16)
    gates = jnp.dot(hidden, gate_weight, preferred_element_type=F32)
    d_attended = (output_grad.astype(F32) * gates * jax.nn.sigmoid(gates)).astype(BF16)

    probs, back_values = pl.pallas_call(
        functools.partial(probs_kernel, held),
        out_shape=(
            jax.ShapeDtypeStruct((tokens, per_block * span), F32),
            jax.ShapeDtypeStruct((owners, span, width), BF16),
        ),
        in_specs=[SMEM, VMEM, VMEM, VMEM],
        out_specs=(VMEM, VMEM),
        name="probs",
    )(ids, queries, d_attended, came_keys)
    came_dvalues = exchange(back_values)

    piece = depth // owners
    half_tokens = jax.ShapeDtypeStruct((tokens // 2, width), BF16)
    keep_dq, keep_dg, send_dq, send_dg, back_keys = pl.pallas_call(
        functools.partial(grads_kernel, held),
        out_shape=(half_tokens,) * 4 + (jax.ShapeDtypeStruct((owners, span, width), BF16),),
        in_specs=[SMEM, SMEM] + [VMEM] * 7,
        out_specs=(VMEM,) * 5,
        name="grads",
    )(ids, tp, queries, d_attended, gates, output_grad, probs, came_keys, came_values)

    half_held = jax.ShapeDtypeStruct((held // 2, span, width), BF16)
    keep_values, send_values, values_across = pl.pallas_call(
        value_totals_kernel,
        out_shape=(half_held, half_held, jax.ShapeDtypeStruct((width, held * span), BF16)),
        in_specs=[SMEM, SMEM, VMEM],
        out_specs=(VMEM, VMEM, VMEM),
        scratch_shapes=[pltpu.VMEM((held + 1, span, width), F32)],
        name="value_totals",
    )(wanted, tp, came_dvalues)

    came_dkeys = exchange(back_keys)
    tile = 256
    parts = pl.pallas_call(
        weight_kernel,
        grid=(depth // tile,),
        out_shape=jax.ShapeDtypeStruct((owners, piece, width), BF16),
        in_specs=[
            pl.BlockSpec((held * span, tile), lambda i: (0, i)),
            pl.BlockSpec((width, held * span), lambda i: (0, 0)),
        ],
        out_specs=pl.BlockSpec((tile // piece, piece, width), lambda i: (i, 0, 0)),
        name="weight",
    )(store_rows, values_across)
    came_parts = exchange(lax.optimization_barrier((parts, came_dkeys))[0])

    keep_keys, send_keys = pl.pallas_call(
        add_slots_kernel,
        out_shape=(half_held, half_held),
        in_specs=[SMEM, SMEM, VMEM],
        out_specs=(VMEM, VMEM),
        scratch_shapes=[pltpu.VMEM((held + 1, span, width), F32)],
        name="key_totals",
    )(wanted, tp, came_dkeys)
    keep_hidden = back((keep_dq, keep_dg), (query_weight, gate_weight), F32)
    send_hidden = back((send_dq, send_dg), (query_weight, gate_weight), BF16)
    rows = held // 2 * span
    keep_keys, send_keys, keep_values, send_values = (
        t.reshape(rows, width) for t in (keep_keys, send_keys, keep_values, send_values)
    )
    came_parts, keep_keys, send_keys, keep_hidden, send_hidden = lax.optimization_barrier(
        (came_parts, keep_keys, send_keys, keep_hidden, send_hidden)
    )
    summed = jnp.sum(came_parts.astype(F32), axis=0).astype(BF16)
    gathered = exchange(jnp.broadcast_to(summed, came_parts.shape))

    other_values = swap_tp(send_values)
    other_keys = swap_tp(send_keys)
    other_hidden = swap_tp(send_hidden)
    grad_hidden = (keep_hidden + other_hidden.astype(F32)).astype(BF16)
    grad_store = back(
        (keep_keys, other_keys, keep_values, other_values), (key_weight, other_key, value_weight, other_value), BF16
    ).reshape(held // 2, span, depth)
    gathered, grad_hidden, grad_store = lax.optimization_barrier((gathered, grad_hidden, grad_store))
    grad_value_weight = gathered.reshape(depth, width).astype(F32)
    return grad_hidden, grad_store, grad_value_weight


def solution(mesh):
    placed = (
        P("st", None),
        P("st", None, None),
        P("st", None),
        P(None, "tp"),
        P(None, "tp"),
        P(None, "tp"),
        P(None, "tp"),
        P("st", "tp"),
    )

    return jax.shard_map(
        body,
        mesh=mesh,
        in_specs=placed,
        out_specs=(P(("st", "tp"), None), P(("st", "tp"), None, None), P(None, "tp")),
        check_vma=False,
    )
```

```python
import functools

import jax
import jax.numpy as jnp
from jax import lax
from jax.experimental import pallas as pl
from jax.experimental.pallas import tpu as pltpu
from jax.sharding import PartitionSpec as P

HEAD_DIM = 256
PAUSE = 2650
PAUSE_AGAIN = 1300
F32 = jnp.float32
BF16 = jnp.bfloat16
VMEM = pl.BlockSpec(memory_space=pltpu.VMEM)
SMEM = pl.BlockSpec(memory_space=pltpu.SMEM)
ANY = pl.BlockSpec(memory_space=pl.ANY)


def dot(a, b, ca, cb):
    return lax.dot_general(a, b, (((ca,), (cb,)), ((), ())), preferred_element_type=F32)


def swap_tp(x):
    return lax.ppermute(x, "tp", [(0, 1), (1, 0)])


def exchange(x):
    return lax.all_to_all(x, "st", split_axis=0, concat_axis=0, tiled=True)


def request_kernel(held, ids_ref, out_ref):
    per, blocks = ids_ref.shape
    out_ref[...] = jnp.zeros_like(out_ref)
    for b in range(blocks):
        for j in range(per):
            at = ids_ref[j, b]
            owner = lax.div(at, held)
            out_ref[pl.ds(owner, 1)] = jnp.full((1, out_ref.shape[1]), at - owner * held + 1, jnp.int32)


def pick_kernel(wanted_ref, pause_ref, rows_ref, *refs):
    out_ref, wait, sem = refs[-3:]
    if pause_ref is not None:
        wait[...] = lax.fori_loop(0, pause_ref[0], lambda i, c: jnp.tanh(c), jnp.zeros(wait.shape, F32))

    def step(i, carry):
        at = jnp.maximum(wanted_ref[i, 0] - 1, 0)
        pltpu.make_async_copy(rows_ref.at[at], out_ref.at[i], sem).start()
        return carry

    lax.fori_loop(0, out_ref.shape[0], step, 0, unroll=8)
    pltpu.make_async_copy(out_ref, out_ref, sem).wait()


def pick(wanted, pause, rows, *after):
    return pl.pallas_call(
        pick_kernel,
        out_shape=jax.ShapeDtypeStruct((wanted.shape[0], *rows.shape[1:]), rows.dtype),
        in_specs=[SMEM, SMEM, VMEM] + [ANY] * len(after),
        out_specs=ANY,
        scratch_shapes=[pltpu.VMEM((8, 128), F32), pltpu.SemaphoreType.DMA],
        name="pick",
    )(wanted, pause, rows, *after)


def probs_kernel(held, ids_ref, q_ref, da_ref, k_ref, p_ref, dv_ref):
    per, blocks = ids_ref.shape
    rows = q_ref.shape[0] // blocks
    span = k_ref.shape[1]
    scale = HEAD_DIM**-0.5
    for b in range(blocks):
        mine = slice(b * rows, (b + 1) * rows)
        owner = [lax.div(ids_ref[j, b], held) for j in range(per)]
        k = jnp.concatenate([k_ref[o] for o in owner], axis=0)
        s = dot(q_ref[mine], k, 1, 1) * scale
        e = jnp.exp(s - jnp.max(s, axis=1, keepdims=True))
        p = e / jnp.sum(e, axis=1, keepdims=True)
        p_ref[mine] = p
        dv = dot(p.astype(BF16), da_ref[mine], 0, 0).astype(BF16)
        for j in range(per):
            dv_ref[owner[j]] = dv[j * span : (j + 1) * span]


def grads_kernel(held, ids_ref, tp_ref, q_ref, da_ref, g_ref, og_ref, p_ref, k_ref, v_ref, keep_dq, keep_dg, send_dq, send_dg, dk_ref):
    per, blocks = ids_ref.shape
    rows = q_ref.shape[0] // blocks
    span = k_ref.shape[1]
    scale = HEAD_DIM**-0.5
    half = blocks // 2
    for n in range(blocks):
        b = lax.rem(n + half * tp_ref[0], blocks)
        mine = pl.ds(pl.multiple_of(b * rows, rows), rows)
        owner = [lax.div(ids_ref[j, b], held) for j in range(per)]
        k = jnp.concatenate([k_ref[o] for o in owner], axis=0)
        v = jnp.concatenate([v_ref[o] for o in owner], axis=0)
        p = p_ref[mine]
        q = q_ref[mine]
        g = g_ref[mine]
        dp = dot(da_ref[mine], v, 1, 1)
        attended = dot(p.astype(BF16), v, 1, 0)
        centre = jnp.sum(p * dp, axis=1, keepdims=True)
        ds = (p * (dp - centre) * scale).astype(BF16)
        dq = dot(ds, k, 1, 0).astype(BF16)
        dk = dot(ds, q, 0, 0).astype(BF16)
        sg = jax.nn.sigmoid(g)
        dg = (og_ref[mine].astype(F32) * attended * sg * (1.0 + g * (1.0 - sg))).astype(BF16)
        for j in range(per):
            dk_ref[owner[j]] = dk[j * span : (j + 1) * span]
        at = slice((n % half) * rows, (n % half + 1) * rows)
        (keep_dq if n < half else send_dq)[at] = dq
        (keep_dg if n < half else send_dg)[at] = dg


def add_slots(wanted_ref, tp_ref, came_ref, acc, keep_ref, send_ref):
    acc[...] = jnp.zeros_like(acc)

    def step(i, carry):
        at = wanted_ref[i, 0]
        acc[at] = acc[at] + came_ref[i].astype(F32)
        return carry

    lax.fori_loop(0, came_ref.shape[0], step, 0, unroll=8)
    half = keep_ref.shape[0]
    tp = tp_ref[0]
    keep_ref[...] = acc[pl.ds(1 + half * tp, half)].astype(BF16)
    send_ref[...] = acc[pl.ds(1 + half * (1 - tp), half)].astype(BF16)


def add_slots_kernel(wanted_ref, tp_ref, came_ref, keep_ref, send_ref, acc):
    add_slots(wanted_ref, tp_ref, came_ref, acc, keep_ref, send_ref)


def value_totals_kernel(wanted_ref, tp_ref, came_ref, keep_ref, send_ref, all_ref, acc):
    add_slots(wanted_ref, tp_ref, came_ref, acc, keep_ref, send_ref)
    held, span = acc.shape[0] - 1, acc.shape[1]
    for i in range(held):
        all_ref[:, i * span : (i + 1) * span] = acc[1 + i].T.astype(BF16)


def weight_kernel(store_ref, vt_ref, out_ref):
    part = dot(vt_ref[...], store_ref[...], 1, 0).T.astype(BF16)
    rows = out_ref.shape[1]
    for i in range(out_ref.shape[0]):
        out_ref[i] = part[i * rows : (i + 1) * rows]


def back_kernel(terms, *refs):
    out_ref = refs[-1]
    a = jnp.concatenate([r[...] for r in refs[:terms]], axis=1)
    step = 256
    for n in range(0, out_ref.shape[1], step):
        w = jnp.concatenate([r[n : n + step] for r in refs[terms:-1]], axis=1)
        out_ref[:, n : n + step] = dot(a, w, 1, 1).astype(out_ref.dtype)


def back(terms, weights, dtype, tile=256):
    rows, width = terms[0].shape
    depth = weights[0].shape[0]
    return pl.pallas_call(
        functools.partial(back_kernel, len(terms)),
        grid=(rows // tile,),
        out_shape=jax.ShapeDtypeStruct((rows, depth), dtype),
        in_specs=[pl.BlockSpec((tile, width), lambda i: (i, 0))] * len(terms)
        + [pl.BlockSpec((depth, width), lambda i: (0, 0))] * len(weights),
        out_specs=pl.BlockSpec((tile, depth), lambda i: (i, 0)),
        name="back",
    )(*terms, *weights)


def last_kernel(terms, *refs):
    one_ref, two_ref, out_ref, both_ref = refs[-4:]
    back_kernel(terms, *refs[:-4], out_ref)
    both_ref[...] = (one_ref[...] + two_ref[...].astype(F32)).astype(both_ref.dtype)


def back_and_add(terms, weights, one, two, tile=512):
    rows, width = terms[0].shape
    depth = weights[0].shape[0]
    steps = rows // tile
    thin = pl.BlockSpec((one.shape[0] // steps, depth), lambda i: (i, 0))
    wide = pl.BlockSpec((tile, depth), lambda i: (i, 0))
    return pl.pallas_call(
        functools.partial(last_kernel, len(terms)),
        grid=(steps,),
        out_shape=(jax.ShapeDtypeStruct((rows, depth), BF16), jax.ShapeDtypeStruct(one.shape, BF16)),
        in_specs=[pl.BlockSpec((tile, width), lambda i: (i, 0))] * len(terms)
        + [pl.BlockSpec((depth, width), lambda i: (0, 0))] * len(weights)
        + [thin, thin],
        out_specs=(wide, thin),
        name="last",
    )(*terms, *weights, one, two)


def body(hidden, passage_store, passage_ids, query_weight, gate_weight, key_weight, value_weight, output_grad):
    owners = lax.axis_size("st")
    held, span, depth = passage_store.shape
    _, per_block = passage_ids.shape
    width = query_weight.shape[1]
    tokens = hidden.shape[0]
    tp = lax.axis_index("tp").astype(jnp.int32).reshape(1)

    ids = passage_ids.T
    request = pl.pallas_call(
        functools.partial(request_kernel, held),
        out_shape=jax.ShapeDtypeStruct((owners, 128), jnp.int32),
        in_specs=[SMEM],
        out_specs=VMEM,
        name="request",
    )(ids)
    wanted = exchange(request)

    other_key, other_value = swap_tp(key_weight), swap_tp(value_weight)
    store_rows = passage_store.reshape(held * span, depth)
    keys = jnp.dot(store_rows, key_weight, preferred_element_type=F32).astype(BF16).reshape(held, span, width)
    pause = tp * PAUSE
    came_keys = exchange(pick(wanted, pause, keys, other_key, other_value))
    values = jnp.dot(store_rows, value_weight, preferred_element_type=F32).astype(BF16).reshape(held, span, width)
    came_values = exchange(pick(wanted, tp * PAUSE_AGAIN, values))

    queries = jnp.dot(hidden, query_weight, preferred_element_type=F32).astype(BF16)
    gates = jnp.dot(hidden, gate_weight, preferred_element_type=F32)
    d_attended = (output_grad.astype(F32) * gates * jax.nn.sigmoid(gates)).astype(BF16)

    probs, back_values = pl.pallas_call(
        functools.partial(probs_kernel, held),
        out_shape=(
            jax.ShapeDtypeStruct((tokens, per_block * span), F32),
            jax.ShapeDtypeStruct((owners, span, width), BF16),
        ),
        in_specs=[SMEM, VMEM, VMEM, VMEM],
        out_specs=(VMEM, VMEM),
        name="probs",
    )(ids, queries, d_attended, came_keys)
    came_dvalues = exchange(back_values)

    piece = depth // owners
    half_tokens = jax.ShapeDtypeStruct((tokens // 2, width), BF16)
    keep_dq, keep_dg, send_dq, send_dg, back_keys = pl.pallas_call(
        functools.partial(grads_kernel, held),
        out_shape=(half_tokens,) * 4 + (jax.ShapeDtypeStruct((owners, span, width), BF16),),
        in_specs=[SMEM, SMEM] + [VMEM] * 7,
        out_specs=(VMEM,) * 5,
        name="grads",
    )(ids, tp, queries, d_attended, gates, output_grad, probs, came_keys, came_values)

    keep_hidden = back((keep_dq, keep_dg), (query_weight, gate_weight), F32)
    send_hidden = back((send_dq, send_dg), (query_weight, gate_weight), BF16)

    half_held = jax.ShapeDtypeStruct((held // 2, span, width), BF16)
    keep_values, send_values, values_across = pl.pallas_call(
        value_totals_kernel,
        out_shape=(half_held, half_held, jax.ShapeDtypeStruct((width, held * span), BF16)),
        in_specs=[SMEM, SMEM, VMEM],
        out_specs=(VMEM, VMEM, VMEM),
        scratch_shapes=[pltpu.VMEM((held + 1, span, width), F32)],
        name="value_totals",
    )(wanted, tp, came_dvalues)

    came_dkeys = exchange(back_keys)
    tile = 256
    parts = pl.pallas_call(
        weight_kernel,
        grid=(depth // tile,),
        out_shape=jax.ShapeDtypeStruct((owners, piece, width), BF16),
        in_specs=[
            pl.BlockSpec((held * span, tile), lambda i: (0, i)),
            pl.BlockSpec((width, held * span), lambda i: (0, 0)),
        ],
        out_specs=pl.BlockSpec((tile // piece, piece, width), lambda i: (i, 0, 0)),
        name="weight",
    )(store_rows, values_across)
    came_parts = exchange(lax.optimization_barrier((parts, came_dkeys))[0])

    keep_keys, send_keys = pl.pallas_call(
        add_slots_kernel,
        out_shape=(half_held, half_held),
        in_specs=[SMEM, SMEM, VMEM],
        out_specs=(VMEM, VMEM),
        scratch_shapes=[pltpu.VMEM((held + 1, span, width), F32)],
        name="key_totals",
    )(wanted, tp, came_dkeys)
    rows = held // 2 * span
    keep_keys, send_keys, keep_values, send_values = (
        t.reshape(rows, width) for t in (keep_keys, send_keys, keep_values, send_values)
    )
    came_parts, keep_keys, send_keys = lax.optimization_barrier((came_parts, keep_keys, send_keys))
    summed = jnp.sum(came_parts.astype(F32), axis=0).astype(BF16)
    gathered = exchange(jnp.broadcast_to(summed, came_parts.shape))

    other_values = swap_tp(send_values)
    other_keys = swap_tp(send_keys)
    other_hidden = swap_tp(send_hidden)
    grad_store, grad_hidden = back_and_add(
        (keep_keys, other_keys, keep_values, other_values),
        (key_weight, other_key, value_weight, other_value),
        keep_hidden,
        other_hidden,
    )
    grad_store = grad_store.reshape(held // 2, span, depth)
    gathered, grad_hidden, grad_store = lax.optimization_barrier((gathered, grad_hidden, grad_store))
    grad_value_weight = gathered.reshape(depth, width).astype(F32)
    return grad_hidden, grad_store, grad_value_weight


def solution(mesh):
    placed = (
        P("st", None),
        P("st", None, None),
        P("st", None),
        P(None, "tp"),
        P(None, "tp"),
        P(None, "tp"),
        P(None, "tp"),
        P("st", "tp"),
    )

    return jax.shard_map(
        body,
        mesh=mesh,
        in_specs=placed,
        out_specs=(P(("st", "tp"), None), P(("st", "tp"), None, None), P(None, "tp")),
        check_vma=False,
    )
```

```python
import functools

import jax
import jax.numpy as jnp
from jax import lax
from jax.experimental import pallas as pl
from jax.experimental.pallas import tpu as pltpu
from jax.sharding import PartitionSpec as P

HEAD_DIM = 256
PAUSE = 2900
F32 = jnp.float32
BF16 = jnp.bfloat16
VMEM = pl.BlockSpec(memory_space=pltpu.VMEM)
SMEM = pl.BlockSpec(memory_space=pltpu.SMEM)
ANY = pl.BlockSpec(memory_space=pl.ANY)


def dot(a, b, ca, cb):
    return lax.dot_general(a, b, (((ca,), (cb,)), ((), ())), preferred_element_type=F32)


def swap_tp(x):
    return lax.ppermute(x, "tp", [(0, 1), (1, 0)])


def exchange(x):
    return lax.all_to_all(x, "st", split_axis=0, concat_axis=0, tiled=True)


def request_kernel(held, ids_ref, out_ref):
    per, blocks = ids_ref.shape
    out_ref[...] = jnp.zeros_like(out_ref)
    for b in range(blocks):
        for j in range(per):
            at = ids_ref[j, b]
            owner = lax.div(at, held)
            out_ref[pl.ds(owner, 1)] = jnp.full((1, out_ref.shape[1]), at - owner * held + 1, jnp.int32)


def pick_kernel(wanted_ref, pause_ref, rows_ref, *refs):
    out_ref, wait, sem = refs[-3:]
    if pause_ref is not None:
        wait[...] = lax.fori_loop(0, pause_ref[0], lambda i, c: jnp.tanh(c), jnp.zeros(wait.shape, F32))

    def step(i, carry):
        at = jnp.maximum(wanted_ref[i, 0] - 1, 0)
        pltpu.make_async_copy(rows_ref.at[at], out_ref.at[i], sem).start()
        return carry

    lax.fori_loop(0, out_ref.shape[0], step, 0, unroll=8)
    pltpu.make_async_copy(out_ref, out_ref, sem).wait()


def pick(wanted, pause, rows, *after):
    return pl.pallas_call(
        pick_kernel,
        out_shape=jax.ShapeDtypeStruct((wanted.shape[0], *rows.shape[1:]), rows.dtype),
        in_specs=[SMEM, SMEM, VMEM] + [ANY] * len(after),
        out_specs=ANY,
        scratch_shapes=[pltpu.VMEM((8, 128), F32), pltpu.SemaphoreType.DMA],
        name="pick",
    )(wanted, pause, rows, *after)


def probs_kernel(held, ids_ref, q_ref, da_ref, k_ref, p_ref, dv_ref):
    per, blocks = ids_ref.shape
    rows = q_ref.shape[0] // blocks
    span = k_ref.shape[1]
    scale = HEAD_DIM**-0.5
    for b in range(blocks):
        mine = slice(b * rows, (b + 1) * rows)
        owner = [lax.div(ids_ref[j, b], held) for j in range(per)]
        k = jnp.concatenate([k_ref[o] for o in owner], axis=0)
        s = dot(q_ref[mine], k, 1, 1) * scale
        e = jnp.exp(s - jnp.max(s, axis=1, keepdims=True))
        p = e / jnp.sum(e, axis=1, keepdims=True)
        p_ref[mine] = p
        dv = dot(p.astype(BF16), da_ref[mine], 0, 0).astype(BF16)
        for j in range(per):
            dv_ref[owner[j]] = dv[j * span : (j + 1) * span]


def grads_kernel(held, ids_ref, tp_ref, q_ref, da_ref, g_ref, og_ref, p_ref, k_ref, v_ref, keep_dq, keep_dg, send_dq, send_dg, dk_ref):
    per, blocks = ids_ref.shape
    rows = q_ref.shape[0] // blocks
    span = k_ref.shape[1]
    scale = HEAD_DIM**-0.5
    half = blocks // 2
    for n in range(blocks):
        b = lax.rem(n + half * tp_ref[0], blocks)
        mine = pl.ds(pl.multiple_of(b * rows, rows), rows)
        owner = [lax.div(ids_ref[j, b], held) for j in range(per)]
        k = jnp.concatenate([k_ref[o] for o in owner], axis=0)
        v = jnp.concatenate([v_ref[o] for o in owner], axis=0)
        p = p_ref[mine]
        q = q_ref[mine]
        g = g_ref[mine]
        dp = dot(da_ref[mine], v, 1, 1)
        attended = dot(p.astype(BF16), v, 1, 0)
        centre = jnp.sum(p * dp, axis=1, keepdims=True)
        ds = (p * (dp - centre) * scale).astype(BF16)
        dq = dot(ds, k, 1, 0).astype(BF16)
        dk = dot(ds, q, 0, 0).astype(BF16)
        sg = jax.nn.sigmoid(g)
        dg = (og_ref[mine].astype(F32) * attended * sg * (1.0 + g * (1.0 - sg))).astype(BF16)
        for j in range(per):
            dk_ref[owner[j]] = dk[j * span : (j + 1) * span]
        at = slice((n % half) * rows, (n % half + 1) * rows)
        (keep_dq if n < half else send_dq)[at] = dq
        (keep_dg if n < half else send_dg)[at] = dg


def add_slots(wanted_ref, tp_ref, came_ref, acc, keep_ref, send_ref):
    acc[...] = jnp.zeros_like(acc)

    def step(i, carry):
        at = wanted_ref[i, 0]
        acc[at] = acc[at] + came_ref[i].astype(F32)
        return carry

    lax.fori_loop(0, came_ref.shape[0], step, 0, unroll=8)
    half = keep_ref.shape[0]
    tp = tp_ref[0]
    keep_ref[...] = acc[pl.ds(1 + half * tp, half)].astype(BF16)
    send_ref[...] = acc[pl.ds(1 + half * (1 - tp), half)].astype(BF16)


def add_slots_kernel(wanted_ref, tp_ref, came_ref, keep_ref, send_ref, acc):
    add_slots(wanted_ref, tp_ref, came_ref, acc, keep_ref, send_ref)


def value_totals_kernel(wanted_ref, tp_ref, came_ref, keep_ref, send_ref, all_ref, acc):
    add_slots(wanted_ref, tp_ref, came_ref, acc, keep_ref, send_ref)
    held, span = acc.shape[0] - 1, acc.shape[1]
    for i in range(held):
        all_ref[:, i * span : (i + 1) * span] = acc[1 + i].T.astype(BF16)


def weight_kernel(store_ref, vt_ref, out_ref):
    part = dot(vt_ref[...], store_ref[...], 1, 0).T.astype(BF16)
    rows = out_ref.shape[1]
    for i in range(out_ref.shape[0]):
        out_ref[i] = part[i * rows : (i + 1) * rows]


def back_kernel(terms, *refs):
    out_ref = refs[-1]
    a = jnp.concatenate([r[...] for r in refs[:terms]], axis=1)
    step = 256
    for n in range(0, out_ref.shape[1], step):
        w = jnp.concatenate([r[n : n + step] for r in refs[terms:-1]], axis=1)
        out_ref[:, n : n + step] = dot(a, w, 1, 1).astype(out_ref.dtype)


def back(terms, weights, dtype, tile=256):
    rows, width = terms[0].shape
    depth = weights[0].shape[0]
    return pl.pallas_call(
        functools.partial(back_kernel, len(terms)),
        grid=(rows // tile,),
        out_shape=jax.ShapeDtypeStruct((rows, depth), dtype),
        in_specs=[pl.BlockSpec((tile, width), lambda i: (i, 0))] * len(terms)
        + [pl.BlockSpec((depth, width), lambda i: (0, 0))] * len(weights),
        out_specs=pl.BlockSpec((tile, depth), lambda i: (i, 0)),
        name="back",
    )(*terms, *weights)


def last_kernel(terms, *refs):
    one_ref, two_ref, out_ref, both_ref = refs[-4:]
    back_kernel(terms, *refs[:-4], out_ref)
    both_ref[...] = (one_ref[...] + two_ref[...].astype(F32)).astype(both_ref.dtype)


def back_and_add(terms, weights, one, two, tile=512):
    rows, width = terms[0].shape
    depth = weights[0].shape[0]
    steps = rows // tile
    thin = pl.BlockSpec((one.shape[0] // steps, depth), lambda i: (i, 0))
    wide = pl.BlockSpec((tile, depth), lambda i: (i, 0))
    return pl.pallas_call(
        functools.partial(last_kernel, len(terms)),
        grid=(steps,),
        out_shape=(jax.ShapeDtypeStruct((rows, depth), BF16), jax.ShapeDtypeStruct(one.shape, BF16)),
        in_specs=[pl.BlockSpec((tile, width), lambda i: (i, 0))] * len(terms)
        + [pl.BlockSpec((depth, width), lambda i: (0, 0))] * len(weights)
        + [thin, thin],
        out_specs=(wide, thin),
        name="last",
    )(*terms, *weights, one, two)


def body(hidden, passage_store, passage_ids, query_weight, gate_weight, key_weight, value_weight, output_grad):
    owners = lax.axis_size("st")
    held, span, depth = passage_store.shape
    _, per_block = passage_ids.shape
    width = query_weight.shape[1]
    tokens = hidden.shape[0]
    tp = lax.axis_index("tp").astype(jnp.int32).reshape(1)

    ids = passage_ids.T
    request = pl.pallas_call(
        functools.partial(request_kernel, held),
        out_shape=jax.ShapeDtypeStruct((owners, 128), jnp.int32),
        in_specs=[SMEM],
        out_specs=VMEM,
        name="request",
    )(ids)
    wanted = exchange(request)

    other_key, other_value = swap_tp(key_weight), swap_tp(value_weight)
    store_rows = passage_store.reshape(held * span, depth)
    keys = jnp.dot(store_rows, key_weight, preferred_element_type=F32).astype(BF16).reshape(held, span, width)
    pause = tp * PAUSE
    came_keys = exchange(pick(wanted, pause, keys, other_key, other_value))
    values = jnp.dot(store_rows, value_weight, preferred_element_type=F32).astype(BF16).reshape(held, span, width)
    came_values = exchange(pick(wanted, jnp.zeros_like(tp), values))

    queries = jnp.dot(hidden, query_weight, preferred_element_type=F32).astype(BF16)
    gates = jnp.dot(hidden, gate_weight, preferred_element_type=F32)
    d_attended = (output_grad.astype(F32) * gates * jax.nn.sigmoid(gates)).astype(BF16)

    probs, back_values = pl.pallas_call(
        functools.partial(probs_kernel, held),
        out_shape=(
            jax.ShapeDtypeStruct((tokens, per_block * span), F32),
            jax.ShapeDtypeStruct((owners, span, width), BF16),
        ),
        in_specs=[SMEM, VMEM, VMEM, VMEM],
        out_specs=(VMEM, VMEM),
        name="probs",
    )(ids, queries, d_attended, came_keys)
    came_dvalues = exchange(back_values)

    piece = depth // owners
    half_tokens = jax.ShapeDtypeStruct((tokens // 2, width), BF16)
    keep_dq, keep_dg, send_dq, send_dg, back_keys = pl.pallas_call(
        functools.partial(grads_kernel, held),
        out_shape=(half_tokens,) * 4 + (jax.ShapeDtypeStruct((owners, span, width), BF16),),
        in_specs=[SMEM, SMEM] + [VMEM] * 7,
        out_specs=(VMEM,) * 5,
        name="grads",
    )(ids, tp, queries, d_attended, gates, output_grad, probs, came_keys, came_values)

    keep_hidden = back((keep_dq, keep_dg), (query_weight, gate_weight), F32)
    send_hidden = back((send_dq, send_dg), (query_weight, gate_weight), BF16)

    half_held = jax.ShapeDtypeStruct((held // 2, span, width), BF16)
    keep_values, send_values, values_across = pl.pallas_call(
        value_totals_kernel,
        out_shape=(half_held, half_held, jax.ShapeDtypeStruct((width, held * span), BF16)),
        in_specs=[SMEM, SMEM, VMEM],
        out_specs=(VMEM, VMEM, VMEM),
        scratch_shapes=[pltpu.VMEM((held + 1, span, width), F32)],
        name="value_totals",
    )(wanted, tp, came_dvalues)

    came_dkeys = exchange(back_keys)
    tile = 256
    parts = pl.pallas_call(
        weight_kernel,
        grid=(depth // tile,),
        out_shape=jax.ShapeDtypeStruct((owners, piece, width), BF16),
        in_specs=[
            pl.BlockSpec((held * span, tile), lambda i: (0, i)),
            pl.BlockSpec((width, held * span), lambda i: (0, 0)),
        ],
        out_specs=pl.BlockSpec((tile // piece, piece, width), lambda i: (i, 0, 0)),
        name="weight",
    )(store_rows, values_across)
    came_parts = exchange(lax.optimization_barrier((parts, came_dkeys))[0])

    keep_keys, send_keys = pl.pallas_call(
        add_slots_kernel,
        out_shape=(half_held, half_held),
        in_specs=[SMEM, SMEM, VMEM],
        out_specs=(VMEM, VMEM),
        scratch_shapes=[pltpu.VMEM((held + 1, span, width), F32)],
        name="key_totals",
    )(wanted, tp, came_dkeys)
    rows = held // 2 * span
    keep_keys, send_keys, keep_values, send_values = (
        t.reshape(rows, width) for t in (keep_keys, send_keys, keep_values, send_values)
    )
    came_parts, keep_keys, send_keys = lax.optimization_barrier((came_parts, keep_keys, send_keys))
    summed = jnp.sum(came_parts.astype(F32), axis=0).astype(BF16)
    gathered = exchange(jnp.broadcast_to(summed, came_parts.shape))

    other_values = swap_tp(send_values)
    other_keys = swap_tp(send_keys)
    other_hidden = swap_tp(send_hidden)
    grad_store, grad_hidden = back_and_add(
        (keep_keys, other_keys, keep_values, other_values),
        (key_weight, other_key, value_weight, other_value),
        keep_hidden,
        other_hidden,
    )
    grad_store = grad_store.reshape(held // 2, span, depth)
    gathered, grad_hidden, grad_store = lax.optimization_barrier((gathered, grad_hidden, grad_store))
    grad_value_weight = gathered.reshape(depth, width).astype(F32)
    return grad_hidden, grad_store, grad_value_weight


def solution(mesh):
    placed = (
        P("st", None),
        P("st", None, None),
        P("st", None),
        P(None, "tp"),
        P(None, "tp"),
        P(None, "tp"),
        P(None, "tp"),
        P("st", "tp"),
    )

    return jax.shard_map(
        body,
        mesh=mesh,
        in_specs=placed,
        out_specs=(P(("st", "tp"), None), P(("st", "tp"), None, None), P(None, "tp")),
        check_vma=False,
    )
```
